32 devices in a mesh: sp: 16 (over z, y, core), dp: 2 (over x).
Axes of the slice: x: 2, y: 2, z: 4, core: 2. Of those that a mesh axis runs over, the one named last changes fastest.
Arguments:
- signal: bfloat16 [2, 2048, 1024], P('dp', 'sp'), may hold values from -6 to 6
- pace: float32 [2, 16], P('dp'), may hold values from 0.5 to 2
- log_step: float32 [64], P('sp'), may hold values from -5.52 to -4.42
- a_real: float32 [64, 64], P('sp'), may hold values from -4 to -0.002, as said below
- a_imag: float32 [64, 64], P('sp'), may hold values from 0.5 to 201.06177
- in_map: float32 [64, 2, 64, 16], P('sp'), may hold values from -3 to 3
- out_map: float32 [64, 2, 16, 64], P('sp'), may hold values from -0.5 to 0.5
- skip: float32 [1024], P('sp'), may hold values from -1 to 1
- init_state: float32 [2, 2, 64, 64], P('dp', None, 'sp'), may hold values from -5 to 5
- w_glu: bfloat16 [1024, 1024], P('sp', 'dp'), may hold values from -0.1875 to 0.1875
- b_glu: float32 [1024], replicated, may hold values from -4 to 4
- g_mix: float32 [1024], replicated, may hold values from 0.1 to 1.9
- w_out: bfloat16 [1024, 4096], P('sp', 'dp'), may hold values from -0.1875 to 0.1875
Outputs:
- result: bfloat16 [2, 2048, 4096], P('dp', 'sp')
The draws below stay inside these ranges and needn't reach their ends.
Inputs may be any that keep to these rules, and one draw needn't show every extreme that they name: `a_real`: negative entries; within a group all entries are of one order.
All inputs are finite; a program needn't handle non-finite values.
Results may differ from the reference program's by a relative error of at most 0.0075.
Values may be sent and summed in bfloat16 or wider, within the bound.
No kernel may reach another device: no remote copies, remote signals or barrier semaphores. Data moves between devices by JAX's collectives and lax.ppermute only.
A program may use at most 64 MiB of HBM per device.

```python
import math
import jax
import jax.numpy as jnp
from jax import lax

D = 4096
GROUPS = 64
C = 16
P_SIZE = 64
WIDTH = 1024
LENGTH = 2048
BATCH = 2
SPANS = 16


def draw_a_real(key, part):
    first, second, third = jax.random.split(key, 3)
    share = 0.5
    slow = jax.random.uniform(first, (GROUPS, 1), jnp.float32) < share
    slow_rate = jax.random.uniform(second, (GROUPS, P_SIZE), jnp.float32, 0.002, 0.006)
    fast_rate = jax.random.uniform(third, (GROUPS, P_SIZE), jnp.float32, 1.5, 4.0)
    return -jnp.where(slow, slow_rate, fast_rate)


def block_scale(own_key, extent, pieces, low, high):
    def one(axis_at, shards_of):
        steps = jax.random.uniform(jax.random.fold_in(jax.random.fold_in(own_key, 6), axis_at), (shards_of,), jnp.float32, low / len(pieces), high / len(pieces))
        return jnp.repeat(jnp.exp(steps), extent[axis_at] // shards_of).reshape((-1,) + (1,) * (len(extent) - axis_at - 1))

    level = one(*pieces[0])
    for cut in pieces[1:]:
        level = level * one(*cut)
    return level


def scatter_about(own_key, extent, width, reach, pieces=(), kind=jnp.bfloat16):
    factor_of = block_scale(own_key, extent, pieces, -0.22, 0.18) if pieces else 1.0
    result = jax.random.normal(own_key, extent, jnp.float32) * width * factor_of
    return jnp.minimum(jnp.maximum(result, -reach), reach).astype(kind)


def setup_inputs(seed: int = 0) -> dict:
    seeds = jax.random.split(jax.random.key(seed), 14)
    return {
        "signal": scatter_about(seeds[0], (BATCH, LENGTH, WIDTH), 1.0, 6.0, ((0, 2), (1, 16))),
        "pace": jnp.clip(jnp.exp(math.log(2.0) - 1.3862944 * jax.random.uniform(seeds[1], (BATCH, SPANS), jnp.float32) ** block_scale(seeds[1], (BATCH, SPANS), ((0, 2),), -0.2, 0.2)), 0.5, 2.0),
        "log_step": jnp.clip(-5.52 + 1.0999999 * jax.random.uniform(seeds[2], (GROUPS,), jnp.float32) ** block_scale(seeds[2], (GROUPS,), ((0, 16),), -0.2, 0.2), -5.52, -4.42),
        "a_real": draw_a_real(jax.random.fold_in(seeds[13], 71), 0),
        "a_imag": jnp.clip(0.5 + 200.56177 * jax.random.uniform(seeds[4], (GROUPS, P_SIZE), jnp.float32) ** block_scale(seeds[4], (GROUPS, P_SIZE), ((0, 16),), -0.2, 0.2), 0.5, 201.06177),
        "in_map": scatter_about(seeds[5], (GROUPS, 2, P_SIZE, C), 0.5, 3.0, ((0, 16),), jnp.float32),
        "out_map": scatter_about(seeds[6], (GROUPS, 2, C, P_SIZE), (2 * P_SIZE) ** -0.5, 0.5, ((0, 16),), jnp.float32),
        "skip": jnp.clip(jax.random.uniform(seeds[7], (WIDTH,), jnp.float32, -1.0, 1.0) * block_scale(seeds[7], (WIDTH,), ((0, 16),), -0.4, 0.0), -1.0, 1.0),
        "init_state": scatter_about(seeds[8], (BATCH, 2, GROUPS, P_SIZE), 1.0, 5.0, ((0, 2), (2, 16)), jnp.float32),
        "w_glu": scatter_about(seeds[9], (WIDTH, WIDTH), WIDTH ** -0.5, 0.1875, ((0, 16), (1, 2))),
        "b_glu": scatter_about(seeds[10], (WIDTH,), 1.0, 4.0, (), jnp.float32),
        "g_mix": jnp.clip(1.0 + 0.18 * jax.random.normal(seeds[11], (WIDTH,), jnp.float32), 0.1, 1.9),
        "w_out": scatter_about(seeds[12], (WIDTH, D), WIDTH ** -0.5, 0.1875, ((0, 16), (1, 2))),
    }


def combine(first, second):
    a1r, a1i, b1r, b1i = first
    a2r, a2i, b2r, b2i = second
    return (a2r * a1r - a2i * a1i, a2r * a1i + a2i * a1r, a2r * b1r - a2i * b1i + b2r, a2r * b1i + a2i * b1r + b2i)

def mix_group(series, pace_row, log_rate, a_re, a_im, in_map, out_map, skip_row, init):
    blocks_count = pace_row.shape[0]
    length = series.shape[0]
    span = length // blocks_count
    states = a_re.shape[0]
    steps = (jnp.exp(log_rate) * pace_row)[:, None]
    decay = jnp.exp(a_re * steps)
    bar_re = decay * jnp.cos(a_im * steps)
    bar_im = decay * jnp.sin(a_im * steps)
    modulus = a_re * a_re + a_im * a_im
    coef_re = ((bar_re - 1.0) * a_re + bar_im * a_im) / modulus
    coef_im = (bar_im * a_re - (bar_re - 1.0) * a_im) / modulus
    drive_re = coef_re[..., None] * in_map[0] - coef_im[..., None] * in_map[1]
    drive_im = coef_re[..., None] * in_map[1] + coef_im[..., None] * in_map[0]
    drive = jnp.concatenate([drive_re, drive_im], axis=1).astype(jnp.bfloat16)
    blocks = series.reshape(blocks_count, span, series.shape[1])
    inject = jnp.einsum('ksc,kpc->ksp', blocks.astype(jnp.float32), drive.astype(jnp.float32))
    inject = inject.reshape(length, 2 * states)
    in_re = inject[:, :states]
    in_im = inject[:, states:]
    in_re = in_re.at[0].add(bar_re[0] * init[0] - bar_im[0] * init[1])
    in_im = in_im.at[0].add(bar_re[0] * init[1] + bar_im[0] * init[0])
    step_re = jnp.broadcast_to(bar_re[:, None, :], (blocks_count, span, states)).reshape(length, states)
    step_im = jnp.broadcast_to(bar_im[:, None, :], (blocks_count, span, states)).reshape(length, states)
    scanned = lax.associative_scan(combine, (step_re, step_im, in_re, in_im), axis=0)
    highest = lax.Precision.HIGHEST
    response = jnp.dot(scanned[2], out_map[0].T, precision=highest) - jnp.dot(scanned[3], out_map[1].T, precision=highest)
    response = response + skip_row * series.astype(jnp.float32)
    return jax.nn.gelu(response).astype(jnp.bfloat16)

def reference(signal, pace, log_step, a_real, a_imag, in_map, out_map, skip, init_state, w_glu, b_glu, g_mix, w_out):
    grouped = signal.reshape(BATCH, LENGTH, GROUPS, C)
    skips = skip.reshape(GROUPS, C)

    def per_sequence(index):
        sample = lax.dynamic_index_in_dim(grouped, index, 0, keepdims=False)
        pace_row = lax.dynamic_index_in_dim(pace, index, 0, keepdims=False)
        init_row = lax.dynamic_index_in_dim(init_state, index, 0, keepdims=False)

        def per_group(group):
            series = lax.dynamic_index_in_dim(sample, group, 1, keepdims=False)
            start = lax.dynamic_index_in_dim(init_row, group, 1, keepdims=False)
            return mix_group(series, pace_row, log_step[group], a_real[group], a_imag[group], in_map[group], out_map[group], skips[group], start)
        outputs = lax.map(per_group, jnp.arange(GROUPS, dtype=jnp.int32))
        activated = outputs.transpose(1, 0, 2).reshape(LENGTH, WIDTH)
        gate_pre = jnp.dot(activated, w_glu, preferred_element_type=jnp.float32) + b_glu
        gated = activated.astype(jnp.float32) * jax.nn.sigmoid(gate_pre)
        scale = lax.rsqrt(lax.optimization_barrier(jnp.mean(gated * gated, axis=-1, keepdims=True)) + 1e-06)
        mixed = (gated * scale * g_mix).astype(jnp.bfloat16)
        return jnp.dot(mixed, w_out, preferred_element_type=jnp.float32).astype(jnp.bfloat16)
    return lax.map(per_sequence, jnp.arange(BATCH, dtype=jnp.int32))
```

```python
import functools

import jax
import jax.numpy as jnp
from jax import lax
from jax.experimental import pallas as pl
from jax.experimental.pallas import tpu as pltpu
from jax.sharding import PartitionSpec as P

LANES = 128
OCT = 8
SMALL = 16
AXES = ("sp", "dp")
F32 = jnp.float32
BF16 = jnp.bfloat16
VMEM = pltpu.VMEM
LIMIT = 60 * 1024 * 1024


class Plan:
    def __init__(self, mesh, signal, pace, a_real, w_glu, w_out):
        self.sp = mesh.shape["sp"]
        self.X = mesh.shape["dp"]
        self.C = 2 if self.sp % 2 == 0 else 1
        self.Y = 2 if self.sp % (2 * self.C) == 0 else 1
        self.Q = self.C * self.Y
        self.Z = self.sp // self.Q
        self.T = signal.shape[1]
        self.width = signal.shape[2]
        self.gl = a_real.shape[0]
        self.states = a_real.shape[1]
        self.chl = self.width // self.sp
        self.ch = self.chl // self.gl
        self.ng = self.gl * self.Z
        self.noct = self.ng // OCT
        self.rows = self.Q * self.noct
        self.mine = self.Z * self.chl
        self.maprows = self.gl * self.ch
        self.packed = 2 * self.maprows + 3 * SMALL
        self.wr = w_out.shape[0]
        self.wc = w_out.shape[1] // self.C
        self.gc = w_glu.shape[1]
        if signal.shape[0] != 1 or pace.shape[1] != self.sp or self.ng % OCT:
            raise ValueError("unsupported sizes")
        if self.states * 2 != LANES or self.ch * OCT != LANES or 3 * self.gl >= SMALL:
            raise ValueError("unsupported sizes")

    def place(self):
        s = lax.axis_index("sp")
        x = lax.axis_index("dp")
        q = lax.rem(s, self.Q)
        z = lax.div(s, self.Q)
        c = lax.rem(q, self.C)
        y = lax.div(q, self.C)
        return z, y, c, x, q

    def pairs(self, move):
        out = []
        for s in range(self.sp):
            for x in range(self.X):
                q, z = s % self.Q, s // self.Q
                c, y = q % self.C, q // self.C
                z2, y2, c2, x2 = move(z, y, c, x)
                t = (z2 * self.Y + y2) * self.C + c2
                out.append((s * self.X + x, t * self.X + x2))
        return out

    def shift_z(self, k):
        return self.pairs(lambda z, y, c, x: ((z + k) % self.Z, y, c, x))

    def swap_q(self, j):
        def move(z, y, c, x):
            q = (y * self.C + c) ^ j
            return z, q // self.C, q % self.C, x

        return self.pairs(move)

    def mixed(self, flip):
        def move(z, y, c, x):
            return (z, y ^ 1, c, x) if c ^ flip == 0 else (z, y, c, x ^ 1)

        return self.pairs(move)

    def shift_x(self, k):
        return self.pairs(lambda z, y, c, x: (z, y, c, (x + k) % self.X))

    def roles(self, y, c, x):
        if self.Y == 2 and self.X == 2:
            a = (1 - c) if self.C == 2 else 1
            b = 1 - a
            steps = [(0, 0), (a, b), (b, a), (1, 1)]
            return [(jnp.bitwise_xor(y, dy), jnp.bitwise_xor(x, dx)) for dy, dx in steps]
        out = []
        for m in range(self.X):
            for b in range(self.Y):
                out.append((jnp.bitwise_xor(y, b), lax.rem(x + (self.X - m), self.X)))
        return out

    def quad(self, unit):
        if self.Y == 2 and self.X == 2:
            other = send(unit, self.mixed(0))
            both = jnp.stack([unit, other])
            return [both, send(both, self.mixed(1))]
        both = jnp.stack([unit] + [send(unit, self.swap_q(self.C)) for _ in range(self.Y - 1)])
        return [both] + [send(both, self.shift_x(m)) for m in range(1, self.X)]


def send(value, pairs):
    return lax.ppermute(value, AXES, pairs)


def call(kernel, outs, scratch=(), flops=1_000_000, specs=None, **kw):
    return pl.pallas_call(
        kernel,
        out_shape=outs,
        scratch_shapes=list(scratch),
        **({} if specs is None else {"in_specs": specs}),
        compiler_params=pltpu.CompilerParams(vmem_limit_bytes=LIMIT),
        cost_estimate=pl.CostEstimate(flops=flops, bytes_accessed=1_000_000, transcendentals=0),
        **kw,
    )


def shape(dims, kind):
    return jax.ShapeDtypeStruct(dims, kind)


def pack_kernel(p, sig, in_map, out_map, a_re, a_im, log_step, init, skip, w_out, *rest):
    packed, keep, give = rest[0], rest[1], rest[2]
    pieces = rest[3 : 3 + p.Q]
    held, small = rest[3 + p.Q :]
    _, _, c, _, q = p.place()
    x = sig[0]
    for r in range(p.Q):
        slabs = [x[:, (z * p.Q + r) * p.chl : (z * p.Q + r + 1) * p.chl] for z in range(p.Z)]
        held[r] = jnp.concatenate(slabs, axis=1)
    for j in range(p.Q):
        pieces[j][...] = held[jnp.bitwise_xor(q, j)]
    n = p.maprows
    for g in range(p.gl):
        rows = slice(g * p.ch, (g + 1) * p.ch)
        both = jnp.concatenate([in_map[g, 0].T, in_map[g, 1].T], axis=1)
        packed[rows] = both.astype(BF16)
        both = jnp.concatenate([out_map[g, 0], out_map[g, 1]], axis=1)
        packed[n + g * p.ch : n + (g + 1) * p.ch] = both.astype(BF16)
    small[...] = jnp.zeros_like(small)
    small[0 : p.gl] = jnp.concatenate([a_re[...], a_im[...]], axis=1)
    small[p.gl : 2 * p.gl] = jnp.concatenate([init[0, 0], init[0, 1]], axis=1)
    small[2 * p.gl : 3 * p.gl] = jnp.broadcast_to(log_step[...], (p.gl, LANES))
    small[3 * p.gl : 3 * p.gl + 1, 0 : p.chl] = skip[...]
    value = small[...]
    high = value.astype(BF16)
    left = value - high.astype(F32)
    mid = left.astype(BF16)
    low = (left - mid.astype(F32)).astype(BF16)
    packed[2 * n : 2 * n + SMALL] = high
    packed[2 * n + SMALL : 2 * n + 2 * SMALL] = mid
    packed[2 * n + 2 * SMALL : 2 * n + 3 * SMALL] = low
    keep[...] = w_out[:, pl.ds(pl.multiple_of(c * p.wc, LANES), p.wc)]
    give[...] = w_out[:, pl.ds(pl.multiple_of((p.C - 1 - c) * p.wc, LANES), p.wc)]


def unpack(p, z, parts, prm):
    for k in range(p.Z):
        prm[lax.rem(z + (p.Z - k), p.Z)] = parts[k][...]
    n = 2 * p.maprows
    small = []
    for k in range(p.Z):
        high = prm[k, n : n + SMALL].astype(F32)
        mid = prm[k, n + SMALL : n + 2 * SMALL].astype(F32)
        low = prm[k, n + 2 * SMALL : n + 3 * SMALL].astype(F32)
        small.append(high + mid + low)
    return small


def spread(p, small, base, kind):
    lane = lax.broadcasted_iota(jnp.int32, (1, LANES), 1) < p.states
    out = []
    for o in range(p.noct):
        tiles = []
        for j in range(OCT // 2):
            first, second = (
                small[g // p.gl][base + g % p.gl : base + g % p.gl + 1]
                for g in (o * OCT + 2 * j, o * OCT + 2 * j + 1)
            )
            if kind == 0:
                second = pltpu.roll(second, p.states, 1)
            elif kind == 1:
                first = pltpu.roll(first, p.states, 1)
            tiles.append(jnp.where(lane, first, second))
        out.append(jnp.concatenate(tiles, axis=1))
    return jnp.concatenate(out, axis=0)


def block_matrix(p, prm, start, sign, o, out):
    per = OCT // p.gl
    parts = [prm[k, start : start + p.maprows] for k in range(o * per, (o + 1) * per)]
    x = jnp.concatenate(parts, axis=0).astype(F32)
    dims = (LANES, LANES)
    low = lax.broadcasted_iota(jnp.int32, dims, 1) < p.states
    lane_group = lax.broadcasted_iota(jnp.int32, dims, 1) // p.states
    row_group = lax.broadcasted_iota(jnp.int32, dims, 0) // p.ch
    turned = pltpu.roll(x, p.states, 1)
    real = jnp.where(low, x, turned)
    imag = jnp.where(low, turned, x) * sign
    half = OCT * p.states
    for j in range(OCT // 2):
        hit = row_group == lane_group + 2 * j
        at = j * LANES
        out[o, :, at : at + LANES] = jnp.where(hit, real, 0.0).astype(BF16)
        out[o, :, half + at : half + at + LANES] = jnp.where(hit, imag, 0.0).astype(BF16)


def power(a_re, a_im, span):
    size = jnp.exp(a_re * span)
    return size * jnp.cos(a_im * span), size * jnp.sin(a_im * span)


def times(ar, ai, br, bi):
    return ar * br - ai * bi, ar * bi + ai * br


def scan_kernel(p, pace, *refs):
    parts = refs[: p.Z]
    sigs = refs[p.Z : p.Z + p.Q]
    refs = refs[p.Z + p.Q :]
    outs, refs = refs[: p.Q], refs[p.Q :]
    ends, whole, bars, blocks, prods, starts, omat = refs[:7]
    prm, bmat, scr, order, porder = refs[7:]
    z, _, _, _, q = p.place()
    half = OCT * p.states
    small = unpack(p, z, parts, prm)
    are = spread(p, small, 0, 0)
    aim = spread(p, small, 0, 1)
    rate = jnp.exp(spread(p, small, 2 * p.gl, 2))
    starts[:, :half] = spread(p, small, p.gl, 0)
    starts[:, half:] = spread(p, small, p.gl, 1)
    steps = jnp.concatenate(
        [rate * pace[0, p.Q * z + jnp.bitwise_xor(q, j)] for j in range(p.Q)], axis=0
    )
    ar = jnp.concatenate([are] * p.Q, axis=0)
    ai = jnp.concatenate([aim] * p.Q, axis=0)
    br, bi = power(ar, ai, steps)
    bars[:, :half] = br
    bars[:, half:] = bi
    modulus = ar * ar + ai * ai
    cr = ((br - 1.0) * ar + bi * ai) / modulus
    ci = (bi * ar - (br - 1.0) * ai) / modulus
    pr, pi = power(ar, ai, steps * float(p.T))
    blocks[:, :half] = pr
    blocks[:, half:] = pi
    sums = []
    for k in range(p.Z):
        total = pace[0, p.Q * k]
        for j in range(1, p.Q):
            total = total + pace[0, p.Q * k + j]
        sums.append(rate * (total * float(p.T)))
    for k in range(p.Z):
        wr, wi = power(are, aim, sums[k])
        prods[k, :, :half] = wr
        prods[k, :, half:] = wi
    for o in range(p.noct):
        block_matrix(p, prm, 0, 1.0, o, bmat)
        block_matrix(p, prm, p.maprows, -1.0, o, omat)
    for j in range(p.Q):
        for o in range(p.noct):
            x = sigs[j][:, o * LANES : (o + 1) * LANES]
            got = jnp.dot(x, bmat[o], preferred_element_type=F32)
            r = j * p.noct + o
            for t in range(2 * half // LANES):
                scr[t, pl.ds(r, p.T, stride=p.rows), :] = got[:, t * LANES : (t + 1) * LANES]
    tiles = half // LANES

    def step(t, carry):
        at = pl.ds(pl.multiple_of(t * p.rows, p.rows), p.rows)
        new_re, new_im = [], []
        for m in range(tiles):
            s = slice(m * LANES, (m + 1) * LANES)
            xr = scr[m, at, :]
            xi = scr[tiles + m, at, :]
            sr, si = carry[m], carry[tiles + m]
            ur = cr[:, s] * xr - ci[:, s] * xi
            ui = cr[:, s] * xi + ci[:, s] * xr
            nr = (ur + br[:, s] * sr) - bi[:, s] * si
            ni = (ui + br[:, s] * si) + bi[:, s] * sr
            scr[m, at, :] = nr
            scr[tiles + m, at, :] = ni
            new_re.append(nr)
            new_im.append(ni)
        return tuple(new_re + new_im)

    zero = jnp.zeros((p.rows, LANES), F32)
    last = lax.fori_loop(0, p.T, step, (zero,) * (2 * tiles), unroll=4)
    final = jnp.concatenate(last, axis=1)
    ends[...] = final
    for j in range(p.Q):
        order[j] = final[j * p.noct : (j + 1) * p.noct]
        porder[j, :, :half] = pr[j * p.noct : (j + 1) * p.noct]
        porder[j, :, half:] = pi[j * p.noct : (j + 1) * p.noct]
    got = order[q]
    er, ei = got[:, :half], got[:, half:]
    for b in range(1, p.Q):
        at = jnp.bitwise_xor(q, b)
        got, by = order[at], porder[at]
        er, ei = times(by[:, :half], by[:, half:], er, ei)
        er, ei = er + got[:, :half], ei + got[:, half:]
    whole[:, :half] = er
    whole[:, half:] = ei
    skips = jnp.concatenate([small[k][3 * p.gl : 3 * p.gl + 1, : p.chl] for k in range(p.Z)], axis=1)
    for j in range(p.Q):
        for o in range(p.noct):
            y = answer(p, scr, omat, j, o)
            s = slice(o * LANES, (o + 1) * LANES)
            outs[j][:, s] = y + skips[:, s] * sigs[j][:, s].astype(F32)


def answer(p, scr, omat, j, o):
    r = j * p.noct + o
    n = 2 * OCT * p.states // LANES
    states = jnp.concatenate(
        [scr[t, pl.ds(r, p.T, stride=p.rows), :].astype(BF16) for t in range(n)], axis=1
    )
    return lax.dot_general(
        states, omat[o], (((1,), (1,)), ((), ())), preferred_element_type=F32
    )


def lift_kernel(p, ends, bars, blocks, prods, starts, omat, *refs):
    wholes = refs[: p.Z]
    bases = refs[p.Z : p.Z + p.Q]
    outs = refs[p.Z + p.Q : p.Z + 2 * p.Q]
    scr, seen, order = refs[p.Z + 2 * p.Q :]
    z, _, _, _, q = p.place()
    half = OCT * p.states
    for k in range(p.Z):
        seen[lax.rem(z + (p.Z - k), p.Z)] = wholes[k][...]
    vr, vi = starts[:, :half], starts[:, half:]
    for k in range(p.Z - 1):
        nr, ni = times(prods[k, :, :half], prods[k, :, half:], vr, vi)
        nr, ni = nr + seen[k, :, :half], ni + seen[k, :, half:]
        vr = jnp.where(k < z, nr, vr)
        vi = jnp.where(k < z, ni, vi)
    for j in range(p.Q):
        rows = slice(j * p.noct, (j + 1) * p.noct)
        order[0, j] = ends[rows, :]
        order[1, j] = blocks[rows, :]
    for b in range(p.Q):
        at = jnp.bitwise_xor(q, b)
        order[2, at, :, :half] = vr
        order[2, at, :, half:] = vi
        got, by = order[0, at], order[1, at]
        vr, vi = times(by[:, :half], by[:, half:], vr, vi)
        vr, vi = vr + got[:, :half], vi + got[:, half:]
    begin = jnp.concatenate([order[2, j] for j in range(p.Q)], axis=0)
    tiles = half // LANES
    bar = bars[...]

    def step(t, carry):
        at = pl.ds(pl.multiple_of(t * p.rows, p.rows), p.rows)
        new_re, new_im = [], []
        for m in range(tiles):
            br = bar[:, m * LANES : (m + 1) * LANES]
            bi = bar[:, half + m * LANES : half + (m + 1) * LANES]
            nr, ni = times(br, bi, carry[m], carry[tiles + m])
            scr[m, at, :] = nr
            scr[tiles + m, at, :] = ni
            new_re.append(nr)
            new_im.append(ni)
        return tuple(new_re + new_im)

    first = tuple(begin[:, t * LANES : (t + 1) * LANES] for t in range(2 * tiles))
    lax.fori_loop(0, p.T, step, first, unroll=4)
    for j in range(p.Q):
        for o in range(p.noct):
            s = slice(o * LANES, (o + 1) * LANES)
            v = answer(p, scr, omat, j, o) + bases[j][:, s]
            inner = 0.7978845608028654 * (v + 0.044715 * (v * v * v))
            outs[j][:, s] = (0.5 * v * (1.0 + jnp.tanh(inner))).astype(BF16)


def gate_kernel(p, count, b_glu, g_mix, *refs):
    pieces = refs[: p.Q]
    units = refs[p.Q : p.Q + count]
    out = refs[p.Q + count]
    held, weight = refs[p.Q + count + 1 :]
    z, y, c, x, q = p.place()
    for j in range(p.Q):
        held[jnp.bitwise_xor(q, j)] = pieces[j][...]
    slabs = [
        held[r][:, k * p.chl : (k + 1) * p.chl] for k in range(p.Z) for r in range(p.Q)
    ]
    act = jnp.concatenate(slabs, axis=1)
    per = count // p.C
    for side in range(p.C):
        owner = c if side == 0 else 1 - c
        roles = p.roles(y, owner, x)
        at = 0
        for n in range(per):
            unit = units[side * per + n]
            for i in range(unit.shape[0]):
                ys, xs = roles[at + i]
                for k in range(p.Z):
                    zs = lax.rem(z + (p.Z - k), p.Z)
                    row = ((zs * p.Y + ys) * p.C + owner) * p.wr
                    weight[
                        pl.ds(pl.multiple_of(row, p.wr), p.wr),
                        pl.ds(pl.multiple_of(xs * p.gc, LANES), p.gc),
                    ] = unit[i, k]
            at += unit.shape[0]
    pre = jnp.dot(act, weight[...], preferred_element_type=F32) + b_glu[...]
    gated = act.astype(F32) * jax.nn.sigmoid(pre)
    scale = lax.rsqrt(jnp.mean(gated * gated, axis=-1, keepdims=True) + 1e-06)
    out[...] = (gated * scale * g_mix[...]).astype(BF16)


def project_kernel(p, count, mixed, *refs):
    units = refs[:count]
    out = refs[count]
    (weight,) = refs[count + 1 :]
    z, y, c, x, _ = p.place()
    roles = p.roles(y, c, x)
    per = count // p.Z
    for k in range(p.Z):
        zs = lax.rem(z + (p.Z - k), p.Z)
        at = 0
        for n in range(per):
            unit = units[k * per + n]
            for i in range(unit.shape[0]):
                ys, xs = roles[at + i]
                for h in range(p.C):
                    owner = c if h == 0 else 1 - c
                    row = ((zs * p.Y + ys) * p.C + owner) * p.wr
                    weight[xs, pl.ds(pl.multiple_of(row, p.wr), p.wr), :] = unit[
                        i, h * p.wr : (h + 1) * p.wr
                    ]
            at += unit.shape[0]
    rows = mixed[...]
    for n in range(p.X):
        got = jnp.dot(rows, weight[n], preferred_element_type=F32)
        out[:, n * p.wc : (n + 1) * p.wc] = got.astype(BF16)


def merge_kernel(p, *refs):
    halves, out = refs[: p.C], refs[p.C]
    _, _, c, _, _ = p.place()
    for h in range(p.C):
        owner = c if h == 0 else 1 - c
        for n in range(p.X):
            at = pl.multiple_of((n * p.C + owner) * p.wc, LANES)
            out[0, :, pl.ds(at, p.wc)] = halves[h][:, n * p.wc : (n + 1) * p.wc]


def layer(
    mesh,
    signal,
    pace,
    log_step,
    a_real,
    a_imag,
    in_map,
    out_map,
    skip,
    init_state,
    w_glu,
    b_glu,
    g_mix,
    w_out,
):
    p = Plan(mesh, signal, pace, a_real, w_glu, w_out)
    half = OCT * p.states
    packed, keep, give, *pieces = call(
        functools.partial(pack_kernel, p),
        [shape((p.packed, LANES), BF16), shape((p.wr, p.wc), BF16), shape((p.wr, p.wc), BF16)]
        + [shape((p.T, p.mine), BF16)] * p.Q,
        [VMEM((p.Q, p.T, p.mine), BF16), VMEM((SMALL, LANES), F32)],
    )(
        signal,
        in_map,
        out_map,
        a_real,
        a_imag,
        log_step.reshape(p.gl, 1),
        init_state,
        skip.reshape(1, p.chl),
        w_out,
    )
    unit = keep
    if p.C == 2:
        unit = jnp.concatenate([keep, send(give, p.swap_q(1))], axis=0)
    parts = [packed] + [send(packed, p.shift_z(k)) for k in range(1, p.Z)]
    sigs = [pieces[0]] + [send(pieces[j], p.swap_q(j)) for j in range(1, p.Q)]
    glu = jnp.stack([w_glu] + [send(w_glu, p.shift_z(k)) for k in range(1, p.Z)])
    glu_units = p.quad(glu)
    if p.C == 2:
        glu_units = glu_units + [send(u, p.swap_q(1)) for u in glu_units]
    out_units = []
    for k in range(p.Z):
        out_units += p.quad(unit)
        if k + 1 < p.Z:
            unit = send(unit, p.shift_z(1))

    smem = pl.BlockSpec(memory_space=pltpu.SMEM)
    vmem = pl.BlockSpec(memory_space=VMEM)
    results = call(
        functools.partial(scan_kernel, p),
        [shape((p.T, p.mine), F32)] * p.Q
        + [
            shape((p.rows, 2 * half), F32),
            shape((p.noct, 2 * half), F32),
            shape((p.rows, 2 * half), F32),
            shape((p.rows, 2 * half), F32),
            shape((p.Z, p.noct, 2 * half), F32),
            shape((p.noct, 2 * half), F32),
            shape((p.noct, LANES, 2 * half), BF16),
        ],
        [
            VMEM((p.Z, p.packed, LANES), BF16),
            VMEM((p.noct, LANES, 2 * half), BF16),
            VMEM((2 * half // LANES, p.T * p.rows, LANES), F32),
            VMEM((p.Q, p.noct, 2 * half), F32),
            VMEM((p.Q, p.noct, 2 * half), F32),
        ],
        flops=4_000_000_000,
        specs=[smem] + [vmem] * (p.Z + p.Q),
    )(pace, *parts, *sigs)
    bases, (ends, whole, *rest) = results[: p.Q], results[p.Q :]
    wholes = [whole] + [send(whole, p.shift_z(k)) for k in range(1, p.Z)]
    acts = call(
        functools.partial(lift_kernel, p),
        [shape((p.T, p.mine), BF16)] * p.Q,
        [
            VMEM((2 * half // LANES, p.T * p.rows, LANES), F32),
            VMEM((p.Z, p.noct, 2 * half), F32),
            VMEM((3, p.Q, p.noct, 2 * half), F32),
        ],
        flops=3_000_000_000,
    )(ends, *rest, *wholes, *bases)
    acts = [acts[0]] + [send(acts[j], p.swap_q(j)) for j in range(1, p.Q)]
    mixed = call(
        functools.partial(gate_kernel, p, len(glu_units)),
        shape((p.T, p.width), BF16),
        [VMEM((p.Q, p.T, p.mine), BF16), VMEM((p.width, p.width), BF16)],
        flops=2_000_000_000,
    )(b_glu.reshape(1, -1), g_mix.reshape(1, -1), *acts, *glu_units)
    project = call(
        functools.partial(project_kernel, p, len(out_units)),
        shape((p.T, p.X * p.wc), BF16),
        [VMEM((p.X, p.width, p.wc), BF16)],
        flops=2_000_000_000,
    )
    halves = []
    if p.C == 2:
        halves = [send(project(send(mixed, p.swap_q(1)), *out_units), p.swap_q(1))]
    halves = [project(mixed, *out_units)] + halves
    return call(
        functools.partial(merge_kernel, p), shape((1, p.T, p.X * p.C * p.wc), BF16)
    )(*halves)


def solution(mesh):
    in_specs = (
        P("dp", "sp", None),
        P("dp", None),
        P("sp"),
        P("sp", None),
        P("sp", None),
        P("sp", None, None, None),
        P("sp", None, None, None),
        P("sp"),
        P("dp", None, "sp", None),
        P("sp", "dp"),
        P(),
        P(),
        P("sp", "dp"),
    )
    return jax.shard_map(
        functools.partial(layer, mesh),
        mesh=mesh,
        in_specs=in_specs,
        out_specs=P("dp", "sp", None),
        check_vma=False,
    )
```

```python
import functools

import jax
import jax.numpy as jnp
from jax import lax
from jax.experimental import pallas as pl
from jax.experimental.pallas import tpu as pltpu
from jax.sharding import PartitionSpec as P


LANES = 128
OCT = 8
SMALL = 16
AXES = ("sp", "dp")
F32 = jnp.float32
BF16 = jnp.bfloat16
VMEM = pltpu.VMEM
MIB = 1024 * 1024


class Plan:
    def __init__(self, mesh, signal, pace, a_real, w_glu, w_out):
        self.sp = mesh.shape["sp"]
        self.X = mesh.shape["dp"]
        self.C = 2 if self.sp % 2 == 0 else 1
        self.Y = 2 if self.sp % (2 * self.C) == 0 else 1
        self.Q = self.C * self.Y
        self.Z = self.sp // self.Q
        self.T = signal.shape[1]
        self.width = signal.shape[2]
        self.gl = a_real.shape[0]
        self.states = a_real.shape[1]
        self.chl = self.width // self.sp
        self.ch = self.chl // self.gl
        self.ng = self.gl * self.Z
        self.noct = self.ng // OCT
        self.rows = self.Q * self.noct
        self.mine = self.Z * self.chl
        self.maprows = self.gl * self.ch
        self.packed = 2 * self.maprows + 3 * SMALL
        self.wr = w_out.shape[0]
        self.wc = w_out.shape[1]
        self.mixes = self.Y == 2 and self.X == 2
        self.gc = w_glu.shape[1]
        if signal.shape[0] != 1 or pace.shape[1] != self.sp or self.ng % OCT:
            raise ValueError("unsupported sizes")
        if self.states * 2 != LANES or self.ch * OCT != LANES or 3 * self.gl >= SMALL:
            raise ValueError("unsupported sizes")

    def place(self):
        s = lax.axis_index("sp")
        x = lax.axis_index("dp")
        q = lax.rem(s, self.Q)
        z = lax.div(s, self.Q)
        c = lax.rem(q, self.C)
        y = lax.div(q, self.C)
        return z, y, c, x, q

    def pairs(self, move):
        out = []
        for s in range(self.sp):
            for x in range(self.X):
                q, z = s % self.Q, s // self.Q
                c, y = q % self.C, q // self.C
                z2, y2, c2, x2 = move(z, y, c, x)
                t = (z2 * self.Y + y2) * self.C + c2
                out.append((s * self.X + x, t * self.X + x2))
        return out

    def shift_z(self, k):
        return self.pairs(lambda z, y, c, x: ((z + k) % self.Z, y, c, x))

    def hop_z(self, k):
        if self.Z & (self.Z - 1):
            return self.shift_z(k)
        return self.pairs(lambda z, y, c, x: (z ^ k, y, c, x))

    def hop_source(self, z, k):
        if self.Z & (self.Z - 1):
            return lax.rem(z + (self.Z - k), self.Z)
        return jnp.bitwise_xor(z, k)

    def swap_q(self, j):
        def move(z, y, c, x):
            q = (y * self.C + c) ^ j
            return z, q // self.C, q % self.C, x

        return self.pairs(move)

    def mixed(self, flip):
        def move(z, y, c, x):
            return (z, y ^ 1, c, x) if c ^ flip == 0 else (z, y, c, x ^ 1)

        return self.pairs(move)

    def shift_x(self, k):
        return self.pairs(lambda z, y, c, x: (z, y, c, (x + k) % self.X))

    def roles(self, y, c, x):
        if self.mixes:
            a = (1 - c) if self.C == 2 else 1
            b = 1 - a
            steps = [(0, 0), (a, b), (b, a), (1, 1)]
            return [(jnp.bitwise_xor(y, dy), jnp.bitwise_xor(x, dx)) for dy, dx in steps]
        out = []
        for m in range(self.X):
            for b in range(self.Y):
                out.append((jnp.bitwise_xor(y, b), lax.rem(x + (self.X - m), self.X)))
        return out

    def quad(self, unit):
        if self.mixes:
            both = jnp.stack([unit, send(unit, self.mixed(0))])
            return [both, send(both, self.mixed(1))]
        both = [unit]
        if self.Y == 2:
            both.append(send(unit, self.swap_q(self.C)))
        both = jnp.stack(both)
        return [both] + [send(both, self.shift_x(m)) for m in range(1, self.X)]

    def ring(self, unit):
        out = [unit]
        for _ in range(1, self.Z):
            out.append(send(out[-1], self.shift_z(1)))
        return out

    def other(self, units):
        if self.C == 1:
            return []
        return [send(u, self.swap_q(1)) for u in units]


def send(value, pairs):
    return lax.ppermute(value, AXES, pairs)


def call(mib, kernel, outs, scratch=(), flops=1_000_000, specs=None, **kw):
    return pl.pallas_call(
        kernel,
        out_shape=outs,
        scratch_shapes=list(scratch),
        **({} if specs is None else {"in_specs": specs}),
        compiler_params=pltpu.CompilerParams(vmem_limit_bytes=mib * MIB),
        cost_estimate=pl.CostEstimate(flops=flops, bytes_accessed=1_000_000, transcendentals=0),
        **kw,
    )


def shape(dims, kind):
    return jax.ShapeDtypeStruct(dims, kind)


def pack_kernel(p, log_step, *rest):
    sources, (packed, *pieces) = rest[:7], rest[7 : 8 + p.Q]
    held, small, arrived, *inside = rest[8 + p.Q :]
    copies = [
        pltpu.make_async_copy(source, target, arrived.at[n])
        for n, (source, target) in enumerate(zip(sources, inside))
    ]
    for copy in copies:
        copy.start()
    for copy in copies:
        copy.wait()
    sig, in_map, out_map, a_re, a_im, init, skip = inside
    _, _, _, _, q = p.place()
    x = sig[0]
    for r in range(p.Q):
        slabs = [x[:, (z * p.Q + r) * p.chl : (z * p.Q + r + 1) * p.chl] for z in range(p.Z)]
        held[r] = jnp.concatenate(slabs, axis=1)
    for j in range(p.Q):
        pieces[j][...] = held[jnp.bitwise_xor(q, j)]
    n = p.maprows
    small[...] = jnp.zeros_like(small)
    for g in range(p.gl):
        for at, part in ((0, in_map), (n, out_map)):
            both = jnp.concatenate([part[g, 0], part[g, 1]], axis=1)
            packed[at + g * p.ch : at + (g + 1) * p.ch] = both.astype(BF16)
        small[2 * p.gl + g : 2 * p.gl + g + 1] = jnp.full((1, LANES), log_step[g], F32)
    small[0 : p.gl] = jnp.concatenate([a_re[...], a_im[...]], axis=1)
    small[p.gl : 2 * p.gl] = jnp.concatenate([init[0, 0], init[0, 1]], axis=1)
    small[3 * p.gl : 3 * p.gl + 1, 0 : p.chl] = skip[...]
    value = small[...]
    high = value.astype(BF16)
    left = value - high.astype(F32)
    mid = left.astype(BF16)
    low = (left - mid.astype(F32)).astype(BF16)
    packed[2 * n : 2 * n + SMALL] = high
    packed[2 * n + SMALL : 2 * n + 2 * SMALL] = mid
    packed[2 * n + 2 * SMALL : 2 * n + 3 * SMALL] = low


def unpack(p, z, parts, prm):
    for k in range(p.Z):
        prm[p.hop_source(z, k)] = parts[k][...]
    n = 2 * p.maprows
    small = []
    for k in range(p.Z):
        high = prm[k, n : n + SMALL].astype(F32)
        mid = prm[k, n + SMALL : n + 2 * SMALL].astype(F32)
        low = prm[k, n + 2 * SMALL : n + 3 * SMALL].astype(F32)
        small.append(high + mid + low)
    return small


def spread(p, small, base, kind):
    lane = lax.broadcasted_iota(jnp.int32, (1, LANES), 1) < p.states
    out = []
    for o in range(p.noct):
        tiles = []
        for j in range(OCT // 2):
            first, second = (
                small[g // p.gl][base + g % p.gl : base + g % p.gl + 1]
                for g in (o * OCT + 2 * j, o * OCT + 2 * j + 1)
            )
            if kind == 0:
                second = pltpu.roll(second, p.states, 1)
            elif kind == 1:
                first = pltpu.roll(first, p.states, 1)
            tiles.append(jnp.where(lane, first, second))
        out.append(jnp.concatenate(tiles, axis=1))
    return jnp.concatenate(out, axis=0)


def block_matrix(p, prm, start, sign, o, out):
    per = OCT // p.gl
    parts = [prm[k, start : start + p.maprows] for k in range(o * per, (o + 1) * per)]
    x = jnp.concatenate(parts, axis=0).astype(F32)
    dims = (LANES, LANES)
    low = lax.broadcasted_iota(jnp.int32, dims, 1) < p.states
    lane_group = lax.broadcasted_iota(jnp.int32, dims, 1) // p.states
    row_group = lax.broadcasted_iota(jnp.int32, dims, 0) // p.ch
    turned = pltpu.roll(x, p.states, 1)
    real = jnp.where(low, x, turned)
    imag = jnp.where(low, turned, x) * sign
    half = OCT * p.states
    for j in range(OCT // 2):
        hit = row_group == lane_group + 2 * j
        at = j * LANES
        out[o, :, at : at + LANES] = jnp.where(hit, real, 0.0).astype(BF16)
        out[o, :, half + at : half + at + LANES] = jnp.where(hit, imag, 0.0).astype(BF16)


def power(a_re, a_im, span):
    size = jnp.exp(a_re * span)
    return size * jnp.cos(a_im * span), size * jnp.sin(a_im * span)


def times(ar, ai, br, bi):
    return ar * br - ai * bi, ar * bi + ai * br


def scan_kernel(p, pace, *refs):
    parts = refs[: p.Z]
    sigs = refs[p.Z : p.Z + p.Q]
    refs = refs[p.Z + p.Q :]
    outs, refs = refs[: p.Q], refs[p.Q :]
    ends, whole, bars, blocks, prods, starts, omat = refs[:7]
    prm, bmat, scr, order, porder = refs[7:]
    z, _, _, _, q = p.place()
    half = OCT * p.states
    small = unpack(p, z, parts, prm)
    are = spread(p, small, 0, 0)
    aim = spread(p, small, 0, 1)
    rate = jnp.exp(spread(p, small, 2 * p.gl, 2))
    starts[:, :half] = spread(p, small, p.gl, 0)
    starts[:, half:] = spread(p, small, p.gl, 1)
    steps = jnp.concatenate(
        [rate * pace[0, p.Q * z + jnp.bitwise_xor(q, j)] for j in range(p.Q)], axis=0
    )
    ar = jnp.concatenate([are] * p.Q, axis=0)
    ai = jnp.concatenate([aim] * p.Q, axis=0)
    br, bi = power(ar, ai, steps)
    bars[:, :half] = br
    bars[:, half:] = bi
    modulus = ar * ar + ai * ai
    cr = ((br - 1.0) * ar + bi * ai) / modulus
    ci = (bi * ar - (br - 1.0) * ai) / modulus
    pr, pi = power(ar, ai, steps * float(p.T))
    blocks[:, :half] = pr
    blocks[:, half:] = pi
    sums = []
    for k in range(p.Z):
        total = pace[0, p.Q * k]
        for j in range(1, p.Q):
            total = total + pace[0, p.Q * k + j]
        sums.append(rate * (total * float(p.T)))
    for k in range(p.Z):
        wr, wi = power(are, aim, sums[k])
        prods[k, :, :half] = wr
        prods[k, :, half:] = wi
    for o in range(p.noct):
        block_matrix(p, prm, 0, 1.0, o, bmat)
        block_matrix(p, prm, p.maprows, -1.0, o, omat)
    for j in range(p.Q):
        for o in range(p.noct):
            x = sigs[j][:, o * LANES : (o + 1) * LANES]
            got = jnp.dot(x, bmat[o], preferred_element_type=F32)
            r = j * p.noct + o
            for t in range(2 * half // LANES):
                scr[t, pl.ds(r, p.T, stride=p.rows), :] = got[:, t * LANES : (t + 1) * LANES]
    tiles = half // LANES

    def step(t, carry):
        at = pl.ds(pl.multiple_of(t * p.rows, p.rows), p.rows)
        new_re, new_im = [], []
        for m in range(tiles):
            s = slice(m * LANES, (m + 1) * LANES)
            xr = scr[m, at, :]
            xi = scr[tiles + m, at, :]
            sr, si = carry[m], carry[tiles + m]
            ur = cr[:, s] * xr - ci[:, s] * xi
            ui = cr[:, s] * xi + ci[:, s] * xr
            nr = (ur + br[:, s] * sr) - bi[:, s] * si
            ni = (ui + br[:, s] * si) + bi[:, s] * sr
            scr[m, at, :] = nr
            scr[tiles + m, at, :] = ni
            new_re.append(nr)
            new_im.append(ni)
        return tuple(new_re + new_im)

    zero = jnp.zeros((p.rows, LANES), F32)
    last = lax.fori_loop(0, p.T, step, (zero,) * (2 * tiles), unroll=4)
    final = jnp.concatenate(last, axis=1)
    ends[...] = final
    for j in range(p.Q):
        order[j] = final[j * p.noct : (j + 1) * p.noct]
        porder[j, :, :half] = pr[j * p.noct : (j + 1) * p.noct]
        porder[j, :, half:] = pi[j * p.noct : (j + 1) * p.noct]
    got = order[q]
    er, ei = got[:, :half], got[:, half:]
    for b in range(1, p.Q):
        at = jnp.bitwise_xor(q, b)
        got, by = order[at], porder[at]
        er, ei = times(by[:, :half], by[:, half:], er, ei)
        er, ei = er + got[:, :half], ei + got[:, half:]
    whole[:, :half] = er
    whole[:, half:] = ei
    skips = jnp.concatenate([small[k][3 * p.gl : 3 * p.gl + 1, : p.chl] for k in range(p.Z)], axis=1)
    for j in range(p.Q):
        for o in range(p.noct):
            y = answer(p, scr, omat, j, o)
            s = slice(o * LANES, (o + 1) * LANES)
            outs[j][:, s] = y + skips[:, s] * sigs[j][:, s].astype(F32)


def answer(p, scr, omat, j, o):
    r = j * p.noct + o
    n = 2 * OCT * p.states // LANES
    states = jnp.concatenate(
        [scr[t, pl.ds(r, p.T, stride=p.rows), :].astype(BF16) for t in range(n)], axis=1
    )
    return lax.dot_general(
        states, omat[o], (((1,), (1,)), ((), ())), preferred_element_type=F32
    )


def lift_kernel(p, ends, bars, blocks, prods, starts, omat, *refs):
    wholes = refs[: p.Z]
    bases = refs[p.Z : p.Z + p.Q]
    outs = refs[p.Z + p.Q : p.Z + 2 * p.Q]
    scr, seen, order = refs[p.Z + 2 * p.Q :]
    z, _, _, _, q = p.place()
    half = OCT * p.states
    for k in range(p.Z):
        seen[p.hop_source(z, k)] = wholes[k][...]
    vr, vi = starts[:, :half], starts[:, half:]
    for k in range(p.Z - 1):
        nr, ni = times(prods[k, :, :half], prods[k, :, half:], vr, vi)
        nr, ni = nr + seen[k, :, :half], ni + seen[k, :, half:]
        vr = jnp.where(k < z, nr, vr)
        vi = jnp.where(k < z, ni, vi)
    for j in range(p.Q):
        rows = slice(j * p.noct, (j + 1) * p.noct)
        order[0, j] = ends[rows, :]
        order[1, j] = blocks[rows, :]
    for b in range(p.Q):
        at = jnp.bitwise_xor(q, b)
        order[2, at, :, :half] = vr
        order[2, at, :, half:] = vi
        got, by = order[0, at], order[1, at]
        vr, vi = times(by[:, :half], by[:, half:], vr, vi)
        vr, vi = vr + got[:, :half], vi + got[:, half:]
    begin = jnp.concatenate([order[2, j] for j in range(p.Q)], axis=0)
    tiles = half // LANES
    bar = bars[...]

    def step(t, carry):
        at = pl.ds(pl.multiple_of(t * p.rows, p.rows), p.rows)
        new_re, new_im = [], []
        for m in range(tiles):
            br = bar[:, m * LANES : (m + 1) * LANES]
            bi = bar[:, half + m * LANES : half + (m + 1) * LANES]
            nr, ni = times(br, bi, carry[m], carry[tiles + m])
            scr[m, at, :] = nr
            scr[tiles + m, at, :] = ni
            new_re.append(nr)
            new_im.append(ni)
        return tuple(new_re + new_im)

    first = tuple(begin[:, t * LANES : (t + 1) * LANES] for t in range(2 * tiles))
    lax.fori_loop(0, p.T, step, first, unroll=4)
    for j in range(p.Q):
        for o in range(p.noct):
            s = slice(o * LANES, (o + 1) * LANES)
            v = answer(p, scr, omat, j, o) + bases[j][:, s]
            inner = 0.7978845608028654 * (v + 0.044715 * (v * v * v))
            outs[j][:, s] = (0.5 * v * (1.0 + jnp.tanh(inner))).astype(BF16)


def gate_kernel(p, count, b_glu, g_mix, *refs):
    pieces = refs[: p.Q]
    units = refs[p.Q : p.Q + count]
    out = refs[p.Q + count]
    held, weight = refs[p.Q + count + 1 :]
    z, y, c, x, q = p.place()
    for j in range(p.Q):
        held[jnp.bitwise_xor(q, j)] = pieces[j][...]
    slabs = [
        held[r][:, k * p.chl : (k + 1) * p.chl] for k in range(p.Z) for r in range(p.Q)
    ]
    act = jnp.concatenate(slabs, axis=1)
    for side in range(p.C):
        owner = c if side == 0 else 1 - c
        roles = p.roles(y, owner, x)
        for k in range(p.Z):
            unit = units[side * p.Z + k]
            zs = lax.rem(z + (p.Z - k), p.Z)
            for m in range(unit.shape[0]):
                for i in range(unit.shape[1]):
                    ys, xs = roles[m * unit.shape[1] + i]
                    row = pl.multiple_of(((zs * p.Y + ys) * p.C + owner) * p.wr, p.wr)
                    col = pl.multiple_of(xs * p.gc, LANES)
                    weight[pl.ds(row, p.wr), pl.ds(col, p.gc)] = unit[m, i]
    pre = jnp.dot(act, weight[...], preferred_element_type=F32) + b_glu[...]
    gated = act.astype(F32) * jax.nn.sigmoid(pre)
    scale = lax.rsqrt(jnp.mean(gated * gated, axis=-1, keepdims=True) + 1e-06)
    mixed = (gated * scale * g_mix[...]).astype(BF16)
    depth = p.Q * p.wr
    for k in range(p.Z):
        out[k] = mixed[:, k * depth : (k + 1) * depth]


def project_kernel(p, ks, mixed, *refs):
    per = 2 * p.C if p.mixes else p.X * p.C
    units, refs = refs[: per * len(ks)], refs[per * len(ks) :]
    before = None
    if ks[0]:
        before, refs = refs[0], refs[1:]
    out, weight = refs
    z, y, c, x, _ = p.place()
    depth = p.Q * p.wr
    left = []
    for n, k in enumerate(ks):
        zs = lax.rem(z + (p.Z - k), p.Z)
        left.append(mixed[zs])
        for side in range(p.C):
            owner = c if side == 0 else 1 - c
            roles = p.roles(y, owner, x)
            at = 0
            for m in range(per // p.C):
                unit = units[(n * p.C + side) * (per // p.C) + m]
                for i in range(unit.shape[0]):
                    ys, xs = roles[at + i]
                    row = pl.multiple_of((ys * p.C + owner) * p.wr + n * depth, p.wr)
                    col = pl.multiple_of(xs * p.wc, LANES)
                    weight[pl.ds(row, p.wr), pl.ds(col, p.wc)] = unit[i]
                at += unit.shape[0]
    left = jnp.concatenate(left, axis=1)
    wide = 512
    for n in range(p.X * p.wc // wide):
        at = slice(n * wide, (n + 1) * wide)
        got = jnp.dot(left, weight[:, at], preferred_element_type=F32)
        if before is not None:
            got = got + before[:, at]
        if len(out.shape) == 3:
            out[0, :, at] = got.astype(out.dtype)
        else:
            out[:, at] = got


def layer(mesh, *args):
    return body(mesh, *args)


def body(
    mesh,
    signal,
    pace,
    log_step,
    a_real,
    a_imag,
    in_map,
    out_map,
    skip,
    init_state,
    w_glu,
    b_glu,
    g_mix,
    w_out,
):
    p = Plan(mesh, signal, pace, a_real, w_glu, w_out)
    half = OCT * p.states
    smem = pl.BlockSpec(memory_space=pltpu.SMEM)
    vmem = pl.BlockSpec(memory_space=VMEM)
    glu = p.ring(jnp.stack(p.quad(w_glu)))
    glu_units = glu + p.other(glu)
    out_units = []
    for unit in p.ring(w_out):
        units = p.quad(unit)
        out_units.append(units + p.other(units))
    raw = (
        signal,
        in_map.swapaxes(2, 3),
        out_map,
        a_real,
        a_imag,
        init_state,
        skip.reshape(1, p.chl),
    )
    packed, *pieces = call(
        62,
        functools.partial(pack_kernel, p),
        [shape((p.packed, LANES), BF16)] + [shape((p.T, p.mine), BF16)] * p.Q,
        [
            VMEM((p.Q, p.T, p.mine), BF16),
            VMEM((SMALL, LANES), F32),
            pltpu.SemaphoreType.DMA((len(raw),)),
        ]
        + [VMEM(v.shape, v.dtype) for v in raw],
        specs=[smem] + [pl.BlockSpec(memory_space=pltpu.HBM)] * len(raw),
    )(log_step, *raw)
    parts = [packed] + [send(packed, p.hop_z(k)) for k in range(1, p.Z)]
    sigs = [pieces[0]] + [send(pieces[j], p.swap_q(j)) for j in range(1, p.Q)]
    results = call(
        16,
        functools.partial(scan_kernel, p),
        [shape((p.T, p.mine), F32)] * p.Q
        + [
            shape((p.rows, 2 * half), F32),
            shape((p.noct, 2 * half), F32),
            shape((p.rows, 2 * half), F32),
            shape((p.rows, 2 * half), F32),
            shape((p.Z, p.noct, 2 * half), F32),
            shape((p.noct, 2 * half), F32),
            shape((p.noct, LANES, 2 * half), BF16),
        ],
        [
            VMEM((p.Z, p.packed, LANES), BF16),
            VMEM((p.noct, LANES, 2 * half), BF16),
            VMEM((2 * half // LANES, p.T * p.rows, LANES), F32),
            VMEM((p.Q, p.noct, 2 * half), F32),
            VMEM((p.Q, p.noct, 2 * half), F32),
        ],
        flops=4_000_000_000,
        specs=[smem] + [vmem] * (p.Z + p.Q),
    )(pace, *parts, *sigs)
    bases, (ends, whole, *rest) = results[: p.Q], results[p.Q :]
    wholes = [whole] + [send(whole, p.hop_z(k)) for k in range(1, p.Z)]
    acts = call(
        12,
        functools.partial(lift_kernel, p),
        [shape((p.T, p.mine), BF16)] * p.Q,
        [
            VMEM((2 * half // LANES, p.T * p.rows, LANES), F32),
            VMEM((p.Z, p.noct, 2 * half), F32),
            VMEM((3, p.Q, p.noct, 2 * half), F32),
        ],
        flops=3_000_000_000,
    )(ends, *rest, *wholes, *bases)
    acts = [acts[0]] + [send(acts[j], p.swap_q(j)) for j in range(1, p.Q)]
    mixed = call(
        12,
        functools.partial(gate_kernel, p, len(glu_units)),
        shape((p.Z, p.T, p.Q * p.wr), BF16),
        [VMEM((p.Q, p.T, p.mine), BF16), VMEM((p.width, p.width), BF16)],
        flops=2_000_000_000,
    )(b_glu.reshape(1, -1), g_mix.reshape(1, -1), *acts, *glu_units)
    head, tail = tuple(range(p.Z - 1)), (p.Z - 1,)
    depth = p.Q * p.wr
    partial = call(
        24,
        functools.partial(project_kernel, p, head),
        shape((p.T, p.X * p.wc), F32),
        [VMEM((len(head) * depth, p.X * p.wc), BF16)],
        flops=2_000_000_000,
    )(mixed, *[u for k in head for u in out_units[k]])
    return call(
        12,
        functools.partial(project_kernel, p, tail),
        shape((1, p.T, p.X * p.wc), BF16),
        [VMEM((depth, p.X * p.wc), BF16)],
        flops=1_000_000_000,
    )(mixed, *out_units[-1], partial)


def solution(mesh):
    in_specs = (
        P("dp", "sp", None),
        P("dp", None),
        P("sp"),
        P("sp", None),
        P("sp", None),
        P("sp", None, None, None),
        P("sp", None, None, None),
        P("sp"),
        P("dp", None, "sp", None),
        P("sp", "dp"),
        P(),
        P(),
        P("sp", "dp"),
    )
    return jax.shard_map(
        functools.partial(layer, mesh),
        mesh=mesh,
        in_specs=in_specs,
        out_specs=P("dp", "sp", None),
        check_vma=False,
    )
```

```python
import functools

import jax
import jax.numpy as jnp
from jax import lax
from jax.experimental import pallas as pl
from jax.experimental.pallas import tpu as pltpu
from jax.sharding import PartitionSpec as P


LANES = 128
OCT = 8
SMALL = 16
AXES = ("sp", "dp")
F32 = jnp.float32
BF16 = jnp.bfloat16
VMEM = pltpu.VMEM
MIB = 1024 * 1024


class Plan:
    def __init__(self, mesh, signal, pace, a_real, w_glu, w_out):
        self.sp = mesh.shape["sp"]
        self.X = mesh.shape["dp"]
        self.C = 2 if self.sp % 2 == 0 else 1
        self.Y = 2 if self.sp % (2 * self.C) == 0 else 1
        self.Q = self.C * self.Y
        self.Z = self.sp // self.Q
        self.T = signal.shape[1]
        self.width = signal.shape[2]
        self.gl = a_real.shape[0]
        self.states = a_real.shape[1]
        self.chl = self.width // self.sp
        self.ch = self.chl // self.gl
        self.ng = self.gl * self.Z
        self.noct = self.ng // OCT
        self.rows = self.Q * self.noct
        self.mine = self.Z * self.chl
        self.maprows = self.gl * self.ch
        self.packed = 2 * self.maprows + 3 * SMALL
        self.wr = w_out.shape[0]
        self.wc = w_out.shape[1]
        self.mixes = self.Y == 2 and self.X == 2
        self.gc = w_glu.shape[1]
        if signal.shape[0] != 1 or pace.shape[1] != self.sp or self.ng % OCT:
            raise ValueError("unsupported sizes")
        if self.states * 2 != LANES or self.ch * OCT != LANES or 3 * self.gl >= SMALL or self.T & (self.T - 1):
            raise ValueError("unsupported sizes")

    def place(self):
        s = lax.axis_index("sp")
        x = lax.axis_index("dp")
        q = lax.rem(s, self.Q)
        z = lax.div(s, self.Q)
        c = lax.rem(q, self.C)
        y = lax.div(q, self.C)
        return z, y, c, x, q

    def pairs(self, move):
        out = []
        for s in range(self.sp):
            for x in range(self.X):
                q, z = s % self.Q, s // self.Q
                c, y = q % self.C, q // self.C
                z2, y2, c2, x2 = move(z, y, c, x)
                t = (z2 * self.Y + y2) * self.C + c2
                out.append((s * self.X + x, t * self.X + x2))
        return out

    def shift_z(self, k):
        return self.pairs(lambda z, y, c, x: ((z + k) % self.Z, y, c, x))

    def every_z(self, value):
        out = [value]
        for k in range(1, self.Z):
            if self.Z & (self.Z - 1):
                out.append(send(value, self.shift_z(k)))
            else:
                far = self.pairs(lambda z, y, c, x: (z ^ k, y, c, x))
                out.append(send(value, far))
        return out

    def fold(self, i):
        i = i % self.Z
        return 2 * i if 2 * i < self.Z else 2 * (self.Z - i) - 1

    def place_of(self, z):
        return z // 2 if z % 2 == 0 else self.Z - (z + 1) // 2

    def ring_source(self, z, k):
        even = lax.rem(z, 2) == 0
        place = jnp.where(even, lax.div(z, 2), self.Z - lax.div(z + 1, 2))
        place = lax.rem(place + (self.Z - k), self.Z)
        return jnp.where(2 * place < self.Z, 2 * place, 2 * (self.Z - place) - 1)

    def hop_source(self, z, k):
        if self.Z & (self.Z - 1):
            return lax.rem(z + (self.Z - k), self.Z)
        return jnp.bitwise_xor(z, k)

    def settle(self, z, parts, target):
        for k, part in enumerate(parts):
            target[self.hop_source(z, k)] = part[...]

    def swap_q(self, j):
        def move(z, y, c, x):
            q = (y * self.C + c) ^ j
            return z, q // self.C, q % self.C, x

        return self.pairs(move)

    def mixed(self, flip):
        def move(z, y, c, x):
            return (z, y ^ 1, c, x) if c ^ flip == 0 else (z, y, c, x ^ 1)

        return self.pairs(move)

    def shift_x(self, k):
        return self.pairs(lambda z, y, c, x: (z, y, c, (x + k) % self.X))

    def roles(self, y, c, x):
        if self.mixes:
            a = (1 - c) if self.C == 2 else 1
            b = 1 - a
            steps = [(0, 0), (a, b), (b, a), (1, 1)]
            return [(jnp.bitwise_xor(y, dy), jnp.bitwise_xor(x, dx)) for dy, dx in steps]
        out = []
        for m in range(self.X):
            for b in range(self.Y):
                out.append((jnp.bitwise_xor(y, b), lax.rem(x + (self.X - m), self.X)))
        return out

    def quad(self, unit):
        if self.mixes:
            both = jnp.stack([unit, send(unit, self.mixed(0))])
            return [both, send(both, self.mixed(1))]
        both = [unit]
        if self.Y == 2:
            both.append(send(unit, self.swap_q(self.C)))
        both = jnp.stack(both)
        return [both] + [send(both, self.shift_x(m)) for m in range(1, self.X)]

    def ring(self, unit):
        out = [unit]
        step = self.pairs(lambda z, y, c, x: (self.fold(self.place_of(z) + 1), y, c, x))
        for _ in range(1, self.Z):
            out.append(send(out[-1], step))
        return out

    def other(self, units):
        if self.C == 1:
            return []
        return [send(u, self.swap_q(1)) for u in units]


def send(value, pairs):
    return lax.ppermute(value, AXES, pairs)


def call(mib, kernel, outs, scratch=(), flops=1_000_000, specs=None, **kw):
    return pl.pallas_call(
        kernel,
        out_shape=outs,
        scratch_shapes=list(scratch),
        **({} if specs is None else {"in_specs": specs}),
        compiler_params=pltpu.CompilerParams(vmem_limit_bytes=mib * MIB),
        cost_estimate=pl.CostEstimate(flops=flops, bytes_accessed=1_000_000, transcendentals=0),
        **kw,
    )


def shape(dims, kind):
    return jax.ShapeDtypeStruct(dims, kind)


def pack_kernel(p, log_step, *rest):
    sources, (packed, *pieces) = rest[:7], rest[7 : 8 + p.Q]
    held, small, arrived, *inside = rest[8 + p.Q :]
    copies = [
        pltpu.make_async_copy(source, target, arrived.at[n])
        for n, (source, target) in enumerate(zip(sources, inside))
    ]
    for copy in copies:
        copy.start()
    for copy in copies:
        copy.wait()
    sig, in_map, out_map, a_re, a_im, init, skip = inside
    _, _, _, _, q = p.place()
    x = sig[0]
    for r in range(p.Q):
        slabs = [x[:, (z * p.Q + r) * p.chl : (z * p.Q + r + 1) * p.chl] for z in range(p.Z)]
        held[r] = jnp.concatenate(slabs, axis=1)
    for j in range(p.Q):
        pieces[j][...] = held[jnp.bitwise_xor(q, j)]
    n = p.maprows
    small[...] = jnp.zeros_like(small)
    for g in range(p.gl):
        for at, part in ((0, in_map), (n, out_map)):
            both = jnp.concatenate([part[g, 0], part[g, 1]], axis=1)
            packed[at + g * p.ch : at + (g + 1) * p.ch] = both.astype(BF16)
        small[2 * p.gl + g : 2 * p.gl + g + 1] = jnp.full((1, LANES), log_step[g], F32)
    small[0 : p.gl] = jnp.concatenate([a_re[...], a_im[...]], axis=1)
    small[p.gl : 2 * p.gl] = jnp.concatenate([init[0, 0], init[0, 1]], axis=1)
    small[3 * p.gl : 3 * p.gl + 1, 0 : p.chl] = skip[...]
    value = small[...]
    high = value.astype(BF16)
    left = value - high.astype(F32)
    mid = left.astype(BF16)
    low = (left - mid.astype(F32)).astype(BF16)
    packed[2 * n : 2 * n + SMALL] = high
    packed[2 * n + SMALL : 2 * n + 2 * SMALL] = mid
    packed[2 * n + 2 * SMALL : 2 * n + 3 * SMALL] = low


def unpack(p, z, parts, prm):
    p.settle(z, parts, prm)
    n = 2 * p.maprows
    small = []
    for k in range(p.Z):
        high = prm[k, n : n + SMALL].astype(F32)
        mid = prm[k, n + SMALL : n + 2 * SMALL].astype(F32)
        low = prm[k, n + 2 * SMALL : n + 3 * SMALL].astype(F32)
        small.append(high + mid + low)
    return small


def spread(p, small, base, kind):
    lane = lax.broadcasted_iota(jnp.int32, (1, LANES), 1) < p.states
    out = []
    for o in range(p.noct):
        tiles = []
        for j in range(OCT // 2):
            first, second = (
                small[g // p.gl][base + g % p.gl : base + g % p.gl + 1]
                for g in (o * OCT + 2 * j, o * OCT + 2 * j + 1)
            )
            if kind == 0:
                second = pltpu.roll(second, p.states, 1)
            elif kind == 1:
                first = pltpu.roll(first, p.states, 1)
            tiles.append(jnp.where(lane, first, second))
        out.append(jnp.concatenate(tiles, axis=1))
    return jnp.concatenate(out, axis=0)


def block_matrix(p, prm, start, sign, o, out):
    per = OCT // p.gl
    parts = [prm[k, start : start + p.maprows] for k in range(o * per, (o + 1) * per)]
    x = jnp.concatenate(parts, axis=0).astype(F32)
    dims = (LANES, LANES)
    low = lax.broadcasted_iota(jnp.int32, dims, 1) < p.states
    lane_group = lax.broadcasted_iota(jnp.int32, dims, 1) // p.states
    row_group = lax.broadcasted_iota(jnp.int32, dims, 0) // p.ch
    turned = pltpu.roll(x, p.states, 1)
    real = jnp.where(low, x, turned)
    imag = jnp.where(low, turned, x) * sign
    half = OCT * p.states
    for j in range(OCT // 2):
        hit = row_group == lane_group + 2 * j
        at = j * LANES
        out[o, :, at : at + LANES] = jnp.where(hit, real, 0.0).astype(BF16)
        out[o, :, half + at : half + at + LANES] = jnp.where(hit, imag, 0.0).astype(BF16)


def power(a_re, a_im, span):
    size = jnp.exp(a_re * span)
    angle = a_im * span
    turn = jnp.floor(angle * 0.6366197723675814 + 0.5)
    r = ((angle - turn * 1.5703125) - turn * 4.837512969970703e-4) - turn * 7.549789954891882e-8
    r2 = r * r
    sine = r + r * r2 * (-1.6666654611e-1 + r2 * (8.3321608736e-3 + r2 * -1.9515295891e-4))
    even = 4.166664568298827e-2 + r2 * (-1.388731625493765e-3 + r2 * 2.443315711809948e-5)
    cosine = 1.0 - 0.5 * r2 + r2 * r2 * even
    quarter = turn - 4.0 * jnp.floor(turn * 0.25)
    odd = jnp.logical_or(quarter == 1.0, quarter == 3.0)
    s = jnp.where(odd, cosine, sine)
    c = jnp.where(odd, sine, cosine)
    s = jnp.where(quarter >= 2.0, -s, s)
    c = jnp.where(jnp.logical_or(quarter == 1.0, quarter == 2.0), -c, c)
    return size * c, size * s


def times(ar, ai, br, bi):
    return ar * br - ai * bi, ar * bi + ai * br


def scan_kernel(p, count, pace, *refs):
    parts = refs[:count]
    sigs = refs[count : count + p.Q]
    refs = refs[count + p.Q :]
    outs, refs = refs[: p.Q], refs[p.Q :]
    ends, whole, bars, blocks, prods, starts, omat = refs[:7]
    prm, bmat, scr, order, porder = refs[7:]
    z, _, _, _, q = p.place()
    half = OCT * p.states
    small = unpack(p, z, parts, prm)
    are = spread(p, small, 0, 0)
    aim = spread(p, small, 0, 1)
    rate = jnp.exp(spread(p, small, 2 * p.gl, 2))
    starts[:, :half] = spread(p, small, p.gl, 0)
    starts[:, half:] = spread(p, small, p.gl, 1)
    steps = jnp.concatenate(
        [rate * pace[0, p.Q * z + jnp.bitwise_xor(q, j)] for j in range(p.Q)], axis=0
    )
    ar = jnp.concatenate([are] * p.Q, axis=0)
    ai = jnp.concatenate([aim] * p.Q, axis=0)
    br, bi = power(ar, ai, steps)
    bars[:, :half] = br
    bars[:, half:] = bi
    modulus = ar * ar + ai * ai
    cr = ((br - 1.0) * ar + bi * ai) / modulus
    ci = (bi * ar - (br - 1.0) * ai) / modulus
    pr, pi = br, bi
    for _ in range(p.T.bit_length() - 1):
        pr, pi = pr * pr - pi * pi, 2.0 * pr * pi
    blocks[:, :half] = pr
    blocks[:, half:] = pi
    spans = []
    for k in range(p.Z):
        total = pace[0, p.Q * k]
        for j in range(1, p.Q):
            total = total + pace[0, p.Q * k + j]
        spans.append(rate * (total * float(p.T)))
    again = [jnp.concatenate([v] * p.Z, axis=0) for v in (are, aim)]
    wr, wi = power(*again, jnp.concatenate(spans, axis=0))
    for k in range(p.Z):
        prods[k, :, :half] = wr[k * p.noct : (k + 1) * p.noct]
        prods[k, :, half:] = wi[k * p.noct : (k + 1) * p.noct]
    for o in range(p.noct):
        block_matrix(p, prm, 0, 1.0, o, bmat)
        block_matrix(p, prm, p.maprows, -1.0, o, omat)
    for j in range(p.Q):
        for o in range(p.noct):
            x = sigs[j][:, o * LANES : (o + 1) * LANES]
            got = jnp.dot(x, bmat[o], preferred_element_type=F32)
            r = j * p.noct + o
            for t in range(2 * half // LANES):
                scr[t, pl.ds(r, p.T, stride=p.rows), :] = got[:, t * LANES : (t + 1) * LANES]
    tiles = half // LANES

    def step(t, carry):
        at = pl.ds(pl.multiple_of(t * p.rows, p.rows), p.rows)
        new_re, new_im = [], []
        for m in range(tiles):
            s = slice(m * LANES, (m + 1) * LANES)
            xr = scr[m, at, :]
            xi = scr[tiles + m, at, :]
            sr, si = carry[m], carry[tiles + m]
            ur = cr[:, s] * xr - ci[:, s] * xi
            ui = cr[:, s] * xi + ci[:, s] * xr
            nr = (ur + br[:, s] * sr) - bi[:, s] * si
            ni = (ui + br[:, s] * si) + bi[:, s] * sr
            scr[m, at, :] = nr
            scr[tiles + m, at, :] = ni
            new_re.append(nr)
            new_im.append(ni)
        return tuple(new_re + new_im)

    zero = jnp.zeros((p.rows, LANES), F32)
    last = lax.fori_loop(0, p.T, step, (zero,) * (2 * tiles), unroll=4)
    final = jnp.concatenate(last, axis=1)
    ends[...] = final
    for j in range(p.Q):
        order[j] = final[j * p.noct : (j + 1) * p.noct]
        porder[j, :, :half] = pr[j * p.noct : (j + 1) * p.noct]
        porder[j, :, half:] = pi[j * p.noct : (j + 1) * p.noct]
    got = order[q]
    er, ei = got[:, :half], got[:, half:]
    for b in range(1, p.Q):
        at = jnp.bitwise_xor(q, b)
        got, by = order[at], porder[at]
        er, ei = times(by[:, :half], by[:, half:], er, ei)
        er, ei = er + got[:, :half], ei + got[:, half:]
    whole[:, :half] = er
    whole[:, half:] = ei
    skips = jnp.concatenate([small[k][3 * p.gl : 3 * p.gl + 1, : p.chl] for k in range(p.Z)], axis=1)
    for j in range(p.Q):
        for o in range(p.noct):
            y = answer(p, scr, omat, j, o)
            s = slice(o * LANES, (o + 1) * LANES)
            outs[j][:, s] = y + skips[:, s] * sigs[j][:, s].astype(F32)


def answer(p, scr, omat, j, o):
    r = j * p.noct + o
    n = 2 * OCT * p.states // LANES
    states = jnp.concatenate(
        [scr[t, pl.ds(r, p.T, stride=p.rows), :].astype(BF16) for t in range(n)], axis=1
    )
    return lax.dot_general(
        states, omat[o], (((1,), (1,)), ((), ())), preferred_element_type=F32
    )


def lift_kernel(p, count, ends, bars, blocks, prods, starts, omat, *refs):
    wholes, refs = refs[:count], refs[count:]
    bases, outs = refs[: p.Q], refs[p.Q : 2 * p.Q]
    scr, seen, order = refs[2 * p.Q :]
    z, _, _, _, q = p.place()
    half = OCT * p.states
    p.settle(z, wholes, seen)
    vr, vi = starts[:, :half], starts[:, half:]
    for k in range(p.Z - 1):
        nr, ni = times(prods[k, :, :half], prods[k, :, half:], vr, vi)
        nr, ni = nr + seen[k, :, :half], ni + seen[k, :, half:]
        vr = jnp.where(k < z, nr, vr)
        vi = jnp.where(k < z, ni, vi)
    for j in range(p.Q):
        rows = slice(j * p.noct, (j + 1) * p.noct)
        order[0, j] = ends[rows, :]
        order[1, j] = blocks[rows, :]
    for b in range(p.Q):
        at = jnp.bitwise_xor(q, b)
        order[2, at, :, :half] = vr
        order[2, at, :, half:] = vi
        got, by = order[0, at], order[1, at]
        vr, vi = times(by[:, :half], by[:, half:], vr, vi)
        vr, vi = vr + got[:, :half], vi + got[:, half:]
    begin = jnp.concatenate([order[2, j] for j in range(p.Q)], axis=0)
    tiles = half // LANES
    bar = bars[...]

    def step(t, carry):
        at = pl.ds(pl.multiple_of(t * p.rows, p.rows), p.rows)
        new_re, new_im = [], []
        for m in range(tiles):
            br = bar[:, m * LANES : (m + 1) * LANES]
            bi = bar[:, half + m * LANES : half + (m + 1) * LANES]
            nr, ni = times(br, bi, carry[m], carry[tiles + m])
            scr[m, at, :] = nr
            scr[tiles + m, at, :] = ni
            new_re.append(nr)
            new_im.append(ni)
        return tuple(new_re + new_im)

    first = tuple(begin[:, t * LANES : (t + 1) * LANES] for t in range(2 * tiles))
    lax.fori_loop(0, p.T, step, first, unroll=4)
    for j in range(p.Q):
        for o in range(p.noct):
            s = slice(o * LANES, (o + 1) * LANES)
            v = answer(p, scr, omat, j, o) + bases[j][:, s]
            inner = 0.7978845608028654 * (v + 0.044715 * (v * v * v))
            outs[j][:, s] = (0.5 * v * (1.0 + jnp.tanh(inner))).astype(BF16)


def gate_kernel(p, count, b_glu, g_mix, *refs):
    pieces = refs[: p.Q]
    units = refs[p.Q : p.Q + count]
    out = refs[p.Q + count]
    held, weight = refs[p.Q + count + 1 :]
    z, y, c, x, q = p.place()
    for j in range(p.Q):
        held[jnp.bitwise_xor(q, j)] = pieces[j][...]
    slabs = [
        held[r][:, k * p.chl : (k + 1) * p.chl] for k in range(p.Z) for r in range(p.Q)
    ]
    act = jnp.concatenate(slabs, axis=1)
    for side in range(p.C):
        owner = c if side == 0 else 1 - c
        roles = p.roles(y, owner, x)
        for k in range(p.Z):
            unit = units[side * p.Z + k]
            zs = p.ring_source(z, k)
            for m in range(unit.shape[0]):
                for i in range(unit.shape[1]):
                    ys, xs = roles[m * unit.shape[1] + i]
                    row = pl.multiple_of(((zs * p.Y + ys) * p.C + owner) * p.wr, p.wr)
                    col = pl.multiple_of(xs * p.gc, LANES)
                    weight[pl.ds(row, p.wr), pl.ds(col, p.gc)] = unit[m, i]
    pre = jnp.dot(act, weight[...], preferred_element_type=F32) + b_glu[...]
    gated = act.astype(F32) * jax.nn.sigmoid(pre)
    scale = lax.rsqrt(jnp.mean(gated * gated, axis=-1, keepdims=True) + 1e-06)
    mixed = (gated * scale * g_mix[...]).astype(BF16)
    depth = p.Q * p.wr
    for k in range(p.Z):
        out[k] = mixed[:, k * depth : (k + 1) * depth]


def project_kernel(p, ks, mixed, *refs):
    per = 2 * p.C if p.mixes else p.X * p.C
    units, refs = refs[: per * len(ks)], refs[per * len(ks) :]
    before = None
    if ks[0]:
        before, refs = refs[0], refs[1:]
    out, weight = refs
    z, y, c, x, _ = p.place()
    depth = p.Q * p.wr
    left = []
    for n, k in enumerate(ks):
        zs = p.ring_source(z, k)
        left.append(mixed[zs])
        for side in range(p.C):
            owner = c if side == 0 else 1 - c
            roles = p.roles(y, owner, x)
            at = 0
            for m in range(per // p.C):
                unit = units[(n * p.C + side) * (per // p.C) + m]
                for i in range(unit.shape[0]):
                    ys, xs = roles[at + i]
                    row = pl.multiple_of((ys * p.C + owner) * p.wr + n * depth, p.wr)
                    col = pl.multiple_of(xs * p.wc, LANES)
                    weight[pl.ds(row, p.wr), pl.ds(col, p.wc)] = unit[i]
                at += unit.shape[0]
    left = jnp.concatenate(left, axis=1)
    wide = 512
    for n in range(p.X * p.wc // wide):
        at = slice(n * wide, (n + 1) * wide)
        got = jnp.dot(left, weight[:, at], preferred_element_type=F32)
        if before is not None:
            got = got + before[:, at]
        if len(out.shape) == 3:
            out[0, :, at] = got.astype(out.dtype)
        else:
            out[:, at] = got


def layer(mesh, *args):
    return body(mesh, *args)


def body(
    mesh,
    signal,
    pace,
    log_step,
    a_real,
    a_imag,
    in_map,
    out_map,
    skip,
    init_state,
    w_glu,
    b_glu,
    g_mix,
    w_out,
):
    p = Plan(mesh, signal, pace, a_real, w_glu, w_out)
    half = OCT * p.states
    smem = pl.BlockSpec(memory_space=pltpu.SMEM)
    vmem = pl.BlockSpec(memory_space=VMEM)
    glu = p.ring(jnp.stack(p.quad(w_glu)))
    glu_units = glu + p.other(glu)
    out_units = []
    for unit in p.ring(w_out):
        units = p.quad(unit)
        out_units.append(units + p.other(units))
    raw = (
        signal,
        in_map.swapaxes(2, 3),
        out_map,
        a_real,
        a_imag,
        init_state,
        skip.reshape(1, p.chl),
    )
    packed, *pieces = call(
        62,
        functools.partial(pack_kernel, p),
        [shape((p.packed, LANES), BF16)] + [shape((p.T, p.mine), BF16)] * p.Q,
        [
            VMEM((p.Q, p.T, p.mine), BF16),
            VMEM((SMALL, LANES), F32),
            pltpu.SemaphoreType.DMA((len(raw),)),
        ]
        + [VMEM(v.shape, v.dtype) for v in raw],
        specs=[smem] + [pl.BlockSpec(memory_space=pltpu.HBM)] * len(raw),
    )(log_step, *raw)
    parts = p.every_z(packed)
    sigs = [pieces[0]] + [send(pieces[j], p.swap_q(j)) for j in range(1, p.Q)]
    results = call(
        16,
        functools.partial(scan_kernel, p, len(parts)),
        [shape((p.T, p.mine), F32)] * p.Q
        + [
            shape((p.rows, 2 * half), F32),
            shape((p.noct, 2 * half), F32),
            shape((p.rows, 2 * half), F32),
            shape((p.rows, 2 * half), F32),
            shape((p.Z, p.noct, 2 * half), F32),
            shape((p.noct, 2 * half), F32),
            shape((p.noct, LANES, 2 * half), BF16),
        ],
        [
            VMEM((p.Z, p.packed, LANES), BF16),
            VMEM((p.noct, LANES, 2 * half), BF16),
            VMEM((2 * half // LANES, p.T * p.rows, LANES), F32),
            VMEM((p.Q, p.noct, 2 * half), F32),
            VMEM((p.Q, p.noct, 2 * half), F32),
        ],
        flops=4_000_000_000,
        specs=[smem] + [vmem] * (len(parts) + p.Q),
    )(pace, *parts, *sigs)
    bases, (ends, whole, *rest) = results[: p.Q], results[p.Q :]
    wholes = p.every_z(whole)
    acts = call(
        12,
        functools.partial(lift_kernel, p, len(wholes)),
        [shape((p.T, p.mine), BF16)] * p.Q,
        [
            VMEM((2 * half // LANES, p.T * p.rows, LANES), F32),
            VMEM((p.Z, p.noct, 2 * half), F32),
            VMEM((3, p.Q, p.noct, 2 * half), F32),
        ],
        flops=3_000_000_000,
    )(ends, *rest, *wholes, *bases)
    acts = [acts[0]] + [send(acts[j], p.swap_q(j)) for j in range(1, p.Q)]
    mixed = call(
        12,
        functools.partial(gate_kernel, p, len(glu_units)),
        shape((p.Z, p.T, p.Q * p.wr), BF16),
        [VMEM((p.Q, p.T, p.mine), BF16), VMEM((p.width, p.width), BF16)],
        flops=2_000_000_000,
    )(b_glu.reshape(1, -1), g_mix.reshape(1, -1), *acts, *glu_units)
    head, tail = tuple(range(p.Z - 1)), (p.Z - 1,)
    depth = p.Q * p.wr
    partial = call(
        24,
        functools.partial(project_kernel, p, head),
        shape((p.T, p.X * p.wc), F32),
        [VMEM((len(head) * depth, p.X * p.wc), BF16)],
        flops=2_000_000_000,
    )(mixed, *[u for k in head for u in out_units[k]])
    return call(
        12,
        functools.partial(project_kernel, p, tail),
        shape((1, p.T, p.X * p.wc), BF16),
        [VMEM((depth, p.X * p.wc), BF16)],
        flops=1_000_000_000,
    )(mixed, *out_units[-1], partial)


def solution(mesh):
    in_specs = (
        P("dp", "sp", None),
        P("dp", None),
        P("sp"),
        P("sp", None),
        P("sp", None),
        P("sp", None, None, None),
        P("sp", None, None, None),
        P("sp"),
        P("dp", None, "sp", None),
        P("sp", "dp"),
        P(),
        P(),
        P("sp", "dp"),
    )
    return jax.shard_map(
        functools.partial(layer, mesh),
        mesh=mesh,
        in_specs=in_specs,
        out_specs=P("dp", "sp", None),
        check_vma=False,
    )
```
